32 devices in a mesh: fs: 8 (over z, x), tp: 4 (over y, core).
Axes of the slice: x: 2, y: 2, z: 4, core: 2. Of those that a mesh axis runs over, the one named last changes fastest.
Arguments:
- later_input: bfloat16 [6144, 2048], P('fs', 'tp'), may hold values from -6 to 6
- earlier_input: bfloat16 [6144, 2048], P('fs', 'tp'), may hold values from -6 to 6
- cotangent: bfloat16 [6144, 2048], P('fs', 'tp'), may hold values from -6 to 6
- up_weight: bfloat16 [2048, 8192], P('fs', 'tp'), may hold values from -0.125 to 0.125
- down_weight: bfloat16 [8192, 2048], P('tp', 'fs'), may hold values from -0.0625 to 0.0625
- up_running: float32 [2048, 8192], P('fs', 'tp'), may hold values from -6 to 6
- down_running: float32 [2048, 8192], P('fs', 'tp'), may hold values from -6 to 6
Outputs:
- later_output: bfloat16 [6144, 2048], P('fs', 'tp')
- later_preact: bfloat16 [6144, 8192], P('fs', 'tp')
- earlier_grad: bfloat16 [6144, 2048], P('fs', 'tp')
- up_running_out: float32 [2048, 8192], P('fs', 'tp')
- down_running_out: float32 [2048, 8192], P('fs', 'tp')
The draws below stay inside these ranges and needn't reach their ends.
All inputs are finite; a program needn't handle non-finite values.
Results may differ from the reference program's by a relative error of at most 0.014.
Values may be sent and summed in bfloat16 or wider, within the bound.
No kernel may reach another device: no remote copies, remote signals or barrier semaphores. Data moves between devices by JAX's collectives and lax.ppermute only.
A program may use at most 128 MiB of HBM per device.

```python
import jax
import jax.numpy as jnp
from jax import lax

D = 2048
FF = 8192
TOKENS = 6144
N_TP = 4


def with_spikes(values, own_key, source, target, blocks, factor):
    def block_of(axis_at):
        return (jnp.arange(values.shape[axis_at]) // (values.shape[axis_at] // blocks)).reshape((-1,) + (1,) * (values.ndim - 1 - axis_at))

    near = jax.random.permutation(own_key, blocks)[block_of(target)]
    far = (block_of(target) + blocks // 2) % blocks
    return jnp.where((block_of(source) == near) | (block_of(source) == far), factor * values, values)


def steps_of(rng, shape, pieces, least, top_value):
    factor_of, own = 1.0, jax.random.fold_in(rng, 6)
    for position, blocks in pieces:
        steps = jnp.exp(jax.random.uniform(jax.random.fold_in(own, position), (blocks,), jnp.float32, least / len(pieces), top_value / len(pieces)))
        factor_of = factor_of * jnp.repeat(steps, shape[position] // blocks).reshape([-1 if axis == position else 1 for axis in range(len(shape))])
    return factor_of


def scatter_about(key, dims, scale, bound, split=(), kind=jnp.bfloat16):
    result = scale * jax.random.normal(key, dims, jnp.float32)
    if split:
        result = result * steps_of(key, dims, split, -0.22, 0.18)
    return jnp.clip(result, -bound, bound).astype(kind)


def heavy_noise(own_key, dims, scale, reach, split, heavy, held_as=jnp.bfloat16):
    drawn = scale * jax.random.normal(own_key, dims, jnp.float32)
    if split:
        drawn = drawn * steps_of(own_key, dims, split, -0.22, 0.18)
    return jnp.clip(with_spikes(drawn, jax.random.fold_in(own_key, 3), *heavy), -reach, reach).astype(held_as)


def setup_inputs(seed: int = 0) -> dict:
    splits = jax.random.split(jax.random.key(seed), 8)
    return {
        "later_input": scatter_about(splits[0], (TOKENS, D), 1.0, 6.0, ((0, 8), (1, 4))),
        "earlier_input": scatter_about(splits[1], (TOKENS, D), 1.0, 6.0, ((0, 8), (1, 4))),
        "cotangent": heavy_noise(splits[2], (TOKENS, D), 1.0, 6.0, ((0, 8), (1, 4)), (0, 1, 8, 2.0)),
        "up_weight": scatter_about(splits[3], (D, FF), D ** -0.5, 0.125, ((0, 8), (1, 4))),
        "down_weight": scatter_about(splits[4], (FF, D), FF ** -0.5, 0.0625, ((0, 4), (1, 8))),
        "up_running": scatter_about(splits[5], (D, FF), 1.0, 6.0, ((0, 8), (1, 4)), jnp.float32),
        "down_running": scatter_about(splits[6], (D, FF), 1.0, 6.0, ((0, 8), (1, 4)), jnp.float32),
    }


def block_sum(left, right):
    rows = left.shape[0]
    width = left.shape[1] // N_TP
    left_blocks = left.reshape(rows, N_TP, width).transpose(1, 0, 2)
    right_blocks = right.reshape(N_TP, width, right.shape[1])

    def step(total, pair):
        part = jnp.dot(pair[0], pair[1], preferred_element_type=jnp.float32).astype(jnp.bfloat16)
        part = lax.optimization_barrier(part)
        return total + part.astype(jnp.float32), None

    start = jnp.zeros((rows, right.shape[1]), jnp.float32)
    total, _ = lax.scan(step, start, (left_blocks, right_blocks))
    return total.astype(jnp.bfloat16)


def reference(later_input, earlier_input, cotangent, up_weight, down_weight, up_running, down_running):
    later_up = jnp.dot(later_input, up_weight, preferred_element_type=jnp.float32)
    later_preact = later_up.astype(jnp.bfloat16)
    later_hidden = jnp.square(jax.nn.relu(later_up)).astype(jnp.bfloat16)
    later_output = block_sum(later_hidden, down_weight)
    earlier_up = jnp.dot(earlier_input, up_weight, preferred_element_type=jnp.float32)
    earlier_hidden = jnp.square(jax.nn.relu(earlier_up)).astype(jnp.bfloat16)
    hidden_grad = jnp.dot(cotangent, down_weight.T, preferred_element_type=jnp.float32)
    up_grad = (2.0 * jax.nn.relu(earlier_up) * hidden_grad).astype(jnp.bfloat16)
    earlier_grad = block_sum(up_grad, up_weight.T)
    factor = float(TOKENS) ** -0.5
    up_running_out = up_running + jnp.dot(earlier_input.T, up_grad, preferred_element_type=jnp.float32) * factor
    down_running_out = down_running + jnp.dot(cotangent.T, earlier_hidden, preferred_element_type=jnp.float32) * factor
    return later_output, later_preact, earlier_grad, up_running_out, down_running_out
```

```python
import jax
import jax.numpy as jnp
from jax import lax
from jax.experimental import pallas as pl
from jax.experimental.pallas import tpu as pltpu
from jax.sharding import Mesh, PartitionSpec as P


SHARES = (2, 3, 3)
QUEUED = ()
BF, F32 = jnp.bfloat16, jnp.float32
ANY = pl.BlockSpec(memory_space=pl.ANY)


def add(*parts):
    total = parts[0].astype(F32)
    for p in parts[1:]:
        total = total + p.astype(F32)
    return total.astype(BF)


def fence(*values):
    return lax.optimization_barrier(values)


def swap(v, axis):
    return lax.ppermute(v, axis, [(0, 1), (1, 0)])


def dot(p, q, cp, cq):
    return lax.dot_general(p, q, (((cp,), (cq,)), ((), ())), preferred_element_type=F32)


def aligned(v, by):
    return pl.multiple_of(v, by)


def assemble(pieces, spots, shape, Y):
    def kernel(*refs):
        out, mid, into, back = refs[-4:]
        x, y, c = (lax.axis_index(a) for a in "xyc")

        def moves(i):
            ref = refs[i]
            h, w = ref.shape
            r, s, d = spots[i]
            row = aligned((x + r) % 2 * h, h)
            col = aligned(((y + Y - s) % Y * 2 + (c + d) % 2) * w, w)
            return (
                pltpu.make_async_copy(ref, mid.at[i], into.at[i]),
                pltpu.make_async_copy(mid.at[i], out.at[pl.ds(row, h), pl.ds(col, w)], back.at[i]),
            )

        for i in range(len(pieces)):
            moves(i)[0].start()
        for i in range(len(pieces)):
            moves(i)[0].wait()
            moves(i)[1].start()
        for i in range(len(pieces)):
            moves(i)[1].wait()

    m = len(pieces)
    return pl.pallas_call(
        kernel,
        out_shape=jax.ShapeDtypeStruct(shape, BF),
        in_specs=[ANY] * m,
        out_specs=ANY,
        scratch_shapes=[
            pltpu.VMEM((m,) + pieces[0].shape, BF),
            pltpu.SemaphoreType.DMA((m,)),
            pltpu.SemaphoreType.DMA((m,)),
        ],
    )(*pieces)


def place(pair, far, last, fulls, at, width):
    h, ck = pair.shape[-2:]

    def kernel(pair, far, last, *refs):
        wu, wd, o0, o1, mid, into, back = refs[-7:]
        z, y, c = (lax.axis_index(a) for a in "zyc")
        inner = (z == 1) | (z == 2)
        spots = [(i, o, d) for i in (0, 1) for o in (0, 1) for d in (0, 1)]

        def fetch(src, i, o, d):
            return pltpu.make_async_copy(src.at[i, d], mid.at[i, o, d], into.at[i, o, d])

        def store(i, o, d):
            part, whole = ((wu, o0), (wd, o1))[i]
            py = (z // 2 + o) % 2
            row = aligned((py * 2 + d) * h, h)
            rel = aligned(((d + c) % 2 * 2 + (y + py) % 2) * h, h)
            src = mid.at[i, o, d]
            return (
                pltpu.make_async_copy(src, part.at[pl.ds(row, h), :], back.at[i, o, d, 0]),
                pltpu.make_async_copy(
                    src, whole.at[pl.ds(rel, h), pl.ds(at, ck)], back.at[i, o, d, 1]
                ),
            )

        for i, o, d in spots:
            if o == 0:
                fetch(pair, i, o, d).start()

        @pl.when(inner)
        def _():
            for i, o, d in spots:
                if o == 1:
                    fetch(far, i, o, d).start()

        @pl.when(jnp.logical_not(inner))
        def _():
            for i, o, d in spots:
                if o == 1:
                    fetch(last, i, o, d).start()

        for s in spots:
            fetch(far, *s).wait()
            for m in store(*s):
                m.start()
        for s in spots:
            for m in store(*s):
                m.wait()

    one = jax.ShapeDtypeStruct((4 * h, ck), BF)
    whole = jax.ShapeDtypeStruct((4 * h, width), BF)
    old, alias = ([], {}) if fulls is None else (list(fulls), {3: 2, 4: 3})
    wu, wd, f0, f1 = pl.pallas_call(
        kernel,
        out_shape=[one, one, whole, whole],
        in_specs=[ANY] * (3 + len(old)),
        out_specs=[ANY] * 4,
        scratch_shapes=[
            pltpu.VMEM((2, 2, 2, h, ck), BF),
            pltpu.SemaphoreType.DMA((2, 2, 2)),
            pltpu.SemaphoreType.DMA((2, 2, 2, 2)),
        ],
        input_output_aliases=alias,
    )(pair, far, last, *old)
    return wu, wd, (f0, f1)


def on_device(later, earlier, cot, up_w, down_w, up_run, down_run):
    Z, Y = lax.axis_size("z"), lax.axis_size("y")
    z, x, y, c = (lax.axis_index(a) for a in "zxyc")
    rows, feat = later.shape
    kd, cols = up_w.shape
    half = cols // 2
    n = len(SHARES)
    size = [half * s // sum(SHARES) for s in SHARES]
    start = [sum(size[:k]) for k in range(n)]
    model = feat * 2 * Y
    factor = float(rows * 2 * Z) ** (-0.5)
    x0 = x == 0
    short = Z == 4 and Y == 2

    def shift(v, by):
        return lax.ppermute(v, "y", [(i, (i + by) % Y) for i in range(Y)])

    def along_y(v):
        got = [v]
        for _ in range(1, Y):
            got.append(shift(got[-1], 1))
        return got

    def mine(v, axis=0):
        return lax.dynamic_index_in_dim(v, x, axis, keepdims=False)

    def other(v, axis=0):
        return lax.dynamic_index_in_dim(v, 1 - x, axis, keepdims=False)

    def activation(near, far):
        pieces, spots = [], []
        for r, part in ((0, near), (1, far)):
            for s, v in enumerate(part):
                pieces += [v, swap(v, "c")]
                spots += [(r, s, 0), (r, s, 1)]
        return assemble(pieces, spots, (2 * rows, model), Y)

    w2 = jnp.stack((up_w, down_w.T))
    lo, hi = w2[..., :half], w2[..., half:]
    keep, send = jnp.where(x0, lo, hi), jnp.where(x0, hi, lo)
    keep = [keep[..., start[k] : start[k] + size[k]] for k in range(n)]
    send = [send[..., start[k] : start[k] + size[k]] for k in range(n)]

    def joined(k, got):
        return jnp.where(
            x0, jnp.stack((keep[k], got), 1), jnp.stack((got, keep[k]), 1)
        ).reshape(2, 2 * kd, size[k])

    near_pairs = [(0, 1), (1, 0), (2, 3), (3, 2)]

    def gather(b):
        if not short:
            return b, b, b
        even = z % 2 == 0
        near = lax.ppermute(b, "z", near_pairs)
        pair = jnp.where(even, jnp.stack((b, near), 1), jnp.stack((near, b), 1))
        far = lax.ppermute(pair, "z", [(1, 2), (2, 1)])
        return pair, far, lax.ppermute(far, "z", [(1, 0), (2, 3)])

    def reduce_z(k, gu, gd):
        gu, gd = (v.reshape(Z, 2 * kd, -1) for v in (gu, gd))
        g = jnp.stack((gu, gd), 1)
        if not short or k in QUEUED:
            g = g.reshape(Z * 4 * kd, -1)
            return lax.psum_scatter(g, "z", scatter_dimension=0, tiled=True).reshape(2, 2, kd, -1)
        g = g.reshape((2, 2) + g.shape[1:])
        even, up = z % 2 == 0, z // 2
        away = lax.dynamic_index_in_dim(g, 1 - up, 0, keepdims=False)
        got = lax.ppermute(away, "z", [(0, 1), (3, 2)])
        got = lax.ppermute(add(away, got), "z", [(1, 2), (2, 1)])
        home = add(lax.dynamic_index_in_dim(g, up, 0, keepdims=False), got)
        got = lax.ppermute(jnp.where(even, home[1], home[0]), "z", near_pairs)
        return add(jnp.where(even, home[0], home[1]), got).reshape(2, 2, kd, -1)

    def arrive(k, got, fulls):
        if short:
            return place(*got, fulls, start[k], half)
        b = got[0]
        ups, downs = [b], [b]
        for s in range(1, Z):
            ups.append(lax.ppermute(ups[-1], "z", [(i, i + 1) for i in range(s - 1, Z - 1)]))
            downs.append(lax.ppermute(downs[-1], "z", [(i + 1, i) for i in range(Z - s)]))
        full = jnp.zeros((2, Z) + b.shape[1:], BF)
        full = lax.dynamic_update_slice(full, b[:, None], (0, z, 0, 0))
        for s in range(1, Z):
            piece = jnp.where(z >= s, ups[s], downs[Z - s])
            full = lax.dynamic_update_slice(full, piece[:, None], (0, (z - s) % Z, 0, 0))
        full = full.reshape(2, model, size[k])
        rel = full.reshape(2, 2 * Y, feat, size[k])
        rel = [
            lax.dynamic_index_in_dim(rel, (y - s) % Y * 2 + (c + d) % 2, 1, keepdims=False)
            for d in (0, 1)
            for s in range(Y)
        ]
        rel = jnp.concatenate(rel, 1)
        fulls = rel if k == 0 else jnp.concatenate((jnp.stack(fulls_of[0]), rel), 2)
        fulls_of[0] = (fulls[0], fulls[1])
        return full[0], full[1], fulls_of[0]

    fulls_of = [None]

    def compute(k, wu, wd):
        r = jax.nn.relu(dot(ea, wu, 1, 0))
        ug = (2.0 * r * dot(ct, wd, 1, 0)).astype(BF)
        eh = jnp.square(r).astype(BF)
        gu, gd = dot(ea, ug, 0, 0).astype(BF), dot(ct, eh, 0, 0).astype(BF)
        if k == n - 1:
            gu, gd, ug, wu = fence(gu, gd, ug, wu)
        return ug, wu, reduce_z(k, gu, gd)

    def forward(w):
        lu = dot(la, w, 1, 0)
        return lu.astype(BF), jnp.square(jax.nn.relu(lu)).astype(BF)

    wx, wu, wd, ug, red, pre, lh, came, theirs = ([None] * n for _ in range(9))
    got = []
    for k in range(n):
        wx[k] = swap(send[k], "x")
        got.append(gather(joined(k, wx[k])))
    ey = along_y(earlier)
    cy = along_y(cot)
    ea = activation(ey, along_y(swap(earlier, "x")))
    ct = activation(cy, [swap(cot, "x")] + [swap(v, "x") for v in cy[1:]])
    la = activation(along_y(later), along_y(swap(later, "x")))
    fulls = None
    for k in range(n):
        wu[k], wd[k], fulls = arrive(k, got[k], fulls)
        ug[k], wu[k], red[k] = compute(k, wu[k], wd[k])
        pre[k], lh[k] = forward(wu[k])
        came[k] = swap(other(pre[k].reshape(2, rows, -1)), "x")
    ugf, lhf = jnp.concatenate(ug, 1), jnp.concatenate(lh, 1)
    mid = model // 2
    fu, fd = fulls

    def over_y(v):
        m = None
        for r in range(Y - 1, 0, -1):
            p = v[:, r * feat : (r + 1) * feat]
            m = shift(p if m is None else add(p, m), -1)
        return m

    b_away = dot(ugf, fu[mid:], 1, 1).astype(BF)
    b_came = swap(b_away, "c")
    b_sum = add(dot(ugf, fu[:mid], 1, 1), b_came)
    b = add(b_sum[:, :feat], over_y(b_sum)).reshape(2, rows, feat)
    back = add(mine(b), swap(other(b), "x"))
    l_away = dot(lhf, fd[mid:], 1, 1).astype(BF)
    l_came = swap(l_away, "c")
    l_sum = add(dot(lhf, fd[:mid], 1, 1), l_came).reshape(2, rows, -1)
    l = add(mine(l_sum), swap(other(l_sum), "x"))
    out = add(l[:, :feat], over_y(l))

    preact = jnp.zeros((rows, cols), BF)
    for k in range(n):
        own = mine(pre[k].reshape(2, rows, -1))
        for at, v in (
            (start[k], jnp.where(x0, own, came[k])),
            (half + start[k], jnp.where(x0, came[k], own)),
        ):
            preact = lax.dynamic_update_slice(preact, v, (0, at))
    totals = [up_run, down_run]
    for k in range(n):
        theirs[k] = swap(other(red[k], 1), "x")
        own = mine(red[k], 1)
        for i in (0, 1):
            for at, v in (
                (start[k], jnp.where(x0, own[i], theirs[k][i])),
                (half + start[k], jnp.where(x0, theirs[k][i], own[i])),
            ):
                old = lax.slice_in_dim((up_run, down_run)[i], at, at + size[k], axis=1)
                totals[i] = lax.dynamic_update_slice(
                    totals[i], old + v.astype(F32) * factor, (0, at)
                )
    return out, preact, back, *totals


def solution(mesh):
    F, T = mesh.shape["fs"], mesh.shape["tp"]
    fine = Mesh(mesh.devices.reshape(F // 2, 2, T // 2, 2), ("z", "x", "y", "c"))
    s, t = P(("z", "x"), ("y", "c")), P(("y", "c"), ("z", "x"))

    return jax.shard_map(
        on_device,
        mesh=fine,
        in_specs=(s, s, s, s, t, s, s),
        out_specs=(s, s, s, s, s),
        check_vma=False,
    )
```
